512 devices in a mesh: rep: 2 (over z_hi), fs: 32 (over z_lo, y), tp: 8 (over x, core).
Axes of the slice: x: 4, y: 8, z: 8 (z_hi: 2, z_lo: 4; z = z_hi * 4 + z_lo), core: 2. Of those that a mesh axis runs over, the one named last changes fastest.
Arguments:
- tokens: bfloat16 [16384, 2048], P(('rep', 'fs')), may hold values from -6 to 6
- mid_tokens: bfloat16 [16384, 2048], P(('rep', 'fs')), may hold values from -6 to 6
- out_grad: bfloat16 [16384, 2048], P(('rep', 'fs')), may hold values from -16 to 16
- gate_first: bfloat16 [2048, 3072], P('fs', 'tp'), may hold values from -0.125 to 0.125
- up_first: bfloat16 [2048, 3072], P('fs', 'tp'), may hold values from -0.125 to 0.125
- down_first: bfloat16 [3072, 2048], P('tp', 'fs'), may hold values from -0.109375 to 0.109375
- gate_second: bfloat16 [2048, 3072], P('fs', 'tp'), may hold values from -0.125 to 0.125
- up_second: bfloat16 [2048, 3072], P('fs', 'tp'), may hold values from -0.125 to 0.125
- down_second: bfloat16 [3072, 2048], P('tp', 'fs'), may hold values from -0.109375 to 0.109375
Outputs:
- input_grad: bfloat16 [16384, 2048], P(('rep', 'fs'))
- down_grad: float32 [3072, 2048], P('tp', 'fs')
- row_norms: float32 [3072], P('tp')
The draws below stay inside these ranges and needn't reach their ends.
All inputs are finite; a program needn't handle non-finite values.
Results may differ from the reference program's by a relative error of at most 0.025.
Values may be sent and summed in bfloat16 or wider, within the bound.
No kernel may reach another device: no remote copies, remote signals or barrier semaphores. Data moves between devices by JAX's collectives and lax.ppermute only.
A program may use at most 64 MiB of HBM per device.

```python
import jax
import jax.numpy as jnp
from jax import lax

D = 2048
FF = 3072
TOKENS = 16384
N_TP = 8


def strengthened(array, stream_key, source, target, parts, factor):
    def block_of(position):
        return (jnp.arange(array.shape[position]) // (array.shape[position] // parts)).reshape((-1,) + (1,) * (array.ndim - 1 - position))

    first = jax.random.permutation(stream_key, parts)[block_of(target)]
    other_side = (block_of(target) + parts // 2) % parts
    return jnp.where((block_of(source) == first) | (block_of(source) == other_side), factor * array, array)


def level_of(own_key, shape, cuts, smallest, high):
    loudness = 1.0
    for dim, parts in cuts:
        draws = jax.random.uniform(jax.random.fold_in(jax.random.fold_in(own_key, 6), dim), (parts,), jnp.float32, smallest / len(cuts), high / len(cuts))
        loudness = loudness * jnp.repeat(jnp.exp(draws), shape[dim] // parts).reshape((-1,) + (1,) * (len(shape) - 1 - dim))
    return loudness


def gaussian(stream_key, shape, deviation, most, cuts=(), held_as=jnp.bfloat16):
    values = jax.random.normal(stream_key, shape, jnp.float32) * deviation
    if len(cuts) > 0:
        values = level_of(stream_key, shape, cuts, -0.22, 0.18) * values
    return jnp.clip(values, min=-most, max=most).astype(held_as)


def noise_with(rng, shape, scale, most, pieces, heavy, kind=jnp.bfloat16):
    values = scale * jax.random.normal(rng, shape, jnp.float32)
    if pieces:
        values = values * level_of(rng, shape, pieces, -0.22, 0.18)
    return jnp.clip(strengthened(values, jax.random.fold_in(rng, 3), *heavy), -most, most).astype(kind)


def setup_inputs(seed: int = 0) -> dict:
    arg_keys = jax.random.split(jax.random.key(seed), 10)
    return {
        "tokens": gaussian(arg_keys[0], (TOKENS, D), 1.0, 6.0, ((0, 64),)),
        "mid_tokens": gaussian(arg_keys[1], (TOKENS, D), 1.0, 6.0, ((0, 64),)),
        "out_grad": noise_with(arg_keys[2], (TOKENS, D), 1.0, 16.0, ((0, 64),), (0, 1, 64, 4.0)),
        "gate_first": gaussian(arg_keys[3], (D, FF), D ** -0.5, 0.125, ((0, 32), (1, 8))),
        "up_first": gaussian(arg_keys[4], (D, FF), D ** -0.5, 0.125, ((0, 32), (1, 8))),
        "down_first": gaussian(arg_keys[5], (FF, D), FF ** -0.5, 0.109375, ((0, 8), (1, 32))),
        "gate_second": gaussian(arg_keys[6], (D, FF), D ** -0.5, 0.125, ((0, 32), (1, 8))),
        "up_second": gaussian(arg_keys[7], (D, FF), D ** -0.5, 0.125, ((0, 32), (1, 8))),
        "down_second": gaussian(arg_keys[8], (FF, D), FF ** -0.5, 0.109375, ((0, 8), (1, 32))),
    }


eps = 1e-06

def split_partials(d_gate, d_up, gate_w, up_w):
    width = d_gate.shape[1] // N_TP
    total = jnp.zeros((d_gate.shape[0], gate_w.shape[0]), jnp.float32)
    dims = (((1,), (1,)), ((), ()))
    for block in range(N_TP):
        lower = block * width
        part = lax.dot_general(d_gate[:, lower:lower + width], gate_w[:, lower:lower + width], dims, preferred_element_type=jnp.float32)
        part = part + lax.dot_general(d_up[:, lower:lower + width], up_w[:, lower:lower + width], dims, preferred_element_type=jnp.float32)
        rounded = lax.optimization_barrier(part.astype(jnp.bfloat16))
        total = total + rounded.astype(jnp.float32)
    return total

def half_back(field, carried, gate_w, up_w, down_w):
    scale = lax.rsqrt(lax.optimization_barrier(jnp.mean(field * field, axis=1, keepdims=True)) + eps)
    normed = field * scale
    normed_b = normed.astype(jnp.bfloat16)
    gate = jnp.dot(normed_b, gate_w, preferred_element_type=jnp.float32)
    upper = jnp.dot(normed_b, up_w, preferred_element_type=jnp.float32)
    back = 0.5 * lax.dot_general(carried, down_w, (((1,), (1,)), ((), ())), preferred_element_type=jnp.float32)
    logistic = jax.nn.sigmoid(gate)
    activated = gate * logistic
    hidden = (activated * upper).astype(jnp.bfloat16)
    d_gate = (back * upper * logistic * (1.0 + gate * (1.0 - logistic))).astype(jnp.bfloat16)
    d_up = (back * activated).astype(jnp.bfloat16)
    d_normed = split_partials(d_gate, d_up, gate_w, up_w)
    d_field = carried.astype(jnp.float32) + scale * (d_normed - normed * lax.optimization_barrier(jnp.mean(d_normed * normed, axis=1, keepdims=True)))
    return (d_field, hidden)

def reference(tokens, mid_tokens, out_grad, gate_first, up_first, down_first, gate_second, up_second, down_second):
    d_mid, unused = half_back(mid_tokens.astype(jnp.float32), out_grad, gate_second, up_second, down_second)
    mid_grad = d_mid.astype(jnp.bfloat16)
    d_input, hidden = half_back(tokens.astype(jnp.float32), mid_grad, gate_first, up_first, down_first)
    down_grad = 0.5 * lax.dot_general(hidden, mid_grad, (((0,), (0,)), ((), ())), preferred_element_type=jnp.float32)
    row_norms = lax.optimization_barrier(jnp.sum(down_grad * down_grad, axis=1))
    return (d_input.astype(jnp.bfloat16), down_grad, row_norms)
```

```python
import jax
import jax.numpy as jnp
from jax import lax
from jax.sharding import Mesh
from jax.sharding import PartitionSpec as P

FS = ("fs_0", "fs_1")
Z = ("rep", "fs_0")
REP_FS = ("rep", "fs_0", "fs_1")
f32 = jnp.float32
bf16 = jnp.bfloat16

eps = 1e-06


def take_from(value, axis, step):
    n = lax.axis_size(axis)
    return lax.ppermute(value, axis, [((i + step) % n, i) for i in range(n)])


def from_everyone(value, axis):
    n = lax.axis_size(axis)
    return lax.all_to_all(
        jnp.broadcast_to(value[None], (n, *value.shape)), axis, 0, 0, tiled=True
    )


def along_y(value):
    whole = from_everyone(value, "fs_1")
    return whole.reshape(-1, value.shape[1])


def along_z(value):
    half = value.shape[0] // 2
    after = take_from(value, Z, 1)
    before = take_from(value, Z, -1)
    top = take_from(after[:half], Z, 1)
    bottom = take_from(before[half:], Z, -1)
    return ((0, 0, value), (1, 0, after), (3, 0, before), (2, 0, top), (2, half, bottom))


def columns(x, z, piece):
    m, first, w = piece
    span = x.shape[1] // 4
    start = ((z + m) % 4) * span + first
    return lax.dynamic_slice_in_dim(x, start, w.shape[0], axis=1)


def contract(x, z, pieces):
    total = None
    for piece in pieces:
        part = jnp.dot(columns(x, z, piece), piece[2], preferred_element_type=f32)
        total = part if total is None else total + part
    return total


def spread(x, z, pieces):
    dims = (((1,), (1,)), ((), ()))
    out = {
        (m, first): lax.dot_general(x, w, dims, preferred_element_type=f32).astype(bf16)
        for m, first, w in pieces
    }
    half = pieces[3][2].shape[0]
    rel = jnp.concatenate(
        [out[0, 0], out[1, 0], out[2, 0], out[2, half], out[3, 0]], axis=1
    )
    return jnp.roll(rel, z * (2 * half), axis=1)


def swap_cores(value):
    return lax.ppermute(value, "tp", [(i, i ^ 1) for i in range(lax.axis_size("tp"))])


def take_x(value, step):
    n = lax.axis_size("tp")
    return lax.ppermute(value, "tp", [((i + 2 * step) % n, i) for i in range(n)])


def own_rows(partial, core, x):
    rows = partial.shape[0]
    other = lax.dynamic_slice_in_dim(partial, (1 - core) * (rows // 2), rows // 2, axis=0)
    mine = lax.dynamic_slice_in_dim(partial, core * (rows // 2), rows // 2, axis=0)
    chip = (mine.astype(f32) + swap_cores(other).astype(f32)).astype(bf16)
    n = rows // 8

    def block(j):
        return lax.dynamic_slice_in_dim(chip, ((x + j) % 4) * n, n, axis=0)

    total = block(0).astype(f32)
    for j in (1, 3, 2):
        total = total + take_x(block(j), -j).astype(f32)
    return total


def all_rows(value, core, x):
    n = value.shape[0]
    quarter = jnp.concatenate([value] + [take_x(value, j) for j in (1, 2, 3)], axis=0)
    half = jnp.roll(quarter, x * n, axis=0)
    other = swap_cores(half)
    both = jnp.concatenate([half, other], axis=0)
    return jnp.roll(both, core * (4 * n), axis=0)


def half_back(u, c, z, core, x, gate_up, down):
    field = u.astype(f32)
    scale = lax.rsqrt(jnp.mean(field * field, axis=1, keepdims=True) + eps)
    normed_b = (field * scale).astype(bf16)
    both = contract(normed_b, z, gate_up)
    n = both.shape[1] // 2
    gate, upper = both[:, :n], both[:, n:]
    back = 0.5 * contract(c, z, down)
    logistic = jax.nn.sigmoid(gate)
    activated = gate * logistic
    hidden = (activated * upper).astype(bf16)
    d_gate = (back * upper * logistic * (1.0 + gate * (1.0 - logistic))).astype(bf16)
    d_up = (back * activated).astype(bf16)
    partial = spread(jnp.concatenate([d_gate, d_up], axis=1), z, gate_up)
    rows = u.shape[0] // 8
    start = core * (4 * rows) + x * rows
    d_normed = own_rows(partial, core, x)
    field = lax.dynamic_slice_in_dim(u, start, rows, axis=0).astype(f32)
    scale = lax.rsqrt(jnp.mean(field * field, axis=1, keepdims=True) + eps)
    normed = field * scale
    carried = lax.dynamic_slice_in_dim(c, start, rows, axis=0).astype(f32)
    d_field = carried + scale * (
        d_normed - normed * jnp.mean(d_normed * normed, axis=1, keepdims=True)
    )
    return all_rows(d_field.astype(bf16), core, x), hidden


def down_share(hidden, grad, z):
    span = grad.shape[1] // 4
    half = span // 2

    def part(m):
        cols = lax.dynamic_slice_in_dim(grad, ((z + m) % 4) * span, span, axis=1)
        return 0.5 * lax.dot_general(
            cols, hidden, (((0,), (0,)), ((), ())), preferred_element_type=f32
        )

    far = part(2).astype(bf16)
    top = take_from(far[:half], Z, -1).astype(f32)
    bottom = take_from(far[half:], Z, 1).astype(f32)
    after = part(1)
    before = part(3)
    after = jnp.concatenate([after[:half] + top, after[half:]], axis=0).astype(bf16)
    before = jnp.concatenate([before[:half], before[half:] + bottom], axis=0).astype(bf16)
    column = part(0) + take_from(after, Z, -1).astype(f32) + take_from(before, Z, 1).astype(f32)
    column = column.astype(bf16).reshape(lax.axis_size("fs_1"), -1, hidden.shape[1])
    share = lax.all_to_all(column, "fs_1", 0, 0, tiled=True).astype(f32).sum(axis=0)
    share = share.astype(bf16)
    return share.astype(f32) + take_from(share, "rep", 1).astype(f32)


def on_device(
    tokens,
    mid_tokens,
    out_grad,
    gate_first,
    up_first,
    down_first,
    gate_second,
    up_second,
    down_second,
):
    z = lax.axis_index("fs_0")
    tp = lax.axis_index("tp")
    core, x = tp % 2, tp // 2
    gate_up_2 = along_z(along_y(jnp.concatenate([gate_second, up_second], axis=1)))
    down_2 = along_z(along_y(down_second.T))
    gate_up_1 = along_z(along_y(jnp.concatenate([gate_first, up_first], axis=1)))
    down_1 = along_z(along_y(down_first.T))
    mid_grad, _ = half_back(mid_tokens, out_grad, z, core, x, gate_up_2, down_2)
    input_grad, hidden = half_back(tokens, mid_grad, z, core, x, gate_up_1, down_1)
    share = down_share(hidden, mid_grad, z)
    norms = from_everyone(jnp.sum(share * share, axis=0), FS).sum(axis=0)
    return (input_grad, share.T, norms)


def solution(mesh):
    torus = Mesh(
        mesh.devices.reshape(mesh.shape["rep"], 4, 8, mesh.shape["tp"]),
        ("rep", "fs_0", "fs_1", "tp"),
    )
    placed = (
        P(REP_FS, None),
        P(REP_FS, None),
        P(REP_FS, None),
        P(FS, "tp"),
        P(FS, "tp"),
        P("tp", FS),
        P(FS, "tp"),
        P(FS, "tp"),
        P("tp", FS),
    )
    return jax.shard_map(
        on_device,
        mesh=torus,
        in_specs=placed,
        out_specs=(P(REP_FS, None), P("tp", FS), P("tp")),
        check_vma=False,
    )
```

```python
import jax
import jax.numpy as jnp
from jax import lax
from jax.sharding import Mesh
from jax.sharding import PartitionSpec as P

FS = ("fs_0", "fs_1")
Z = ("rep", "fs_0")
REP_FS = ("rep", "fs_0", "fs_1")
f32 = jnp.float32
bf16 = jnp.bfloat16

eps = 1e-06


def take_from(value, axis, step):
    n = lax.axis_size(axis)
    return lax.ppermute(value, axis, [((i + step) % n, i) for i in range(n)])


def from_everyone(value, axis):
    n = lax.axis_size(axis)
    return lax.all_to_all(
        jnp.broadcast_to(value[None], (n, *value.shape)), axis, 0, 0, tiled=True
    )


def along_y(value):
    whole = from_everyone(value, "fs_1")
    return whole.reshape(-1, value.shape[1])


def along_z(value):
    half = value.shape[0] // 2
    next_ = take_from(value, Z, 1)
    last = take_from(value, Z, -1)
    top = take_from(next_[:half], Z, 1)
    bottom = take_from(last[half:], Z, -1)
    return ((0, 0, value), (1, 0, next_), (3, 0, last), (2, 0, top), (2, half, bottom))


def columns(x, z, piece):
    m, first, w = piece
    span = x.shape[1] // 4
    start = ((z + m) % 4) * span + first
    return lax.dynamic_slice_in_dim(x, start, w.shape[0], axis=1)


def contract(x, z, pieces):
    total = None
    for piece in pieces:
        part = jnp.dot(columns(x, z, piece), piece[2], preferred_element_type=f32)
        total = part if total is None else total + part
    return total


def spread(x, z, pieces):
    dims = (((1,), (1,)), ((), ()))
    out = {
        (m, first): lax.dot_general(x, w, dims, preferred_element_type=f32).astype(bf16)
        for m, first, w in pieces
    }
    half = pieces[3][2].shape[0]
    rel = jnp.concatenate(
        [out[0, 0], out[1, 0], out[2, 0], out[2, half], out[3, 0]], axis=1
    )
    return jnp.roll(rel, z * (2 * half), axis=1)


def after(value, *others):
    return lax.optimization_barrier((value, *others))[0]


def own_rows(partial):
    n = lax.axis_size("tp")
    pieces = partial.reshape(n, -1, partial.shape[1])
    return lax.all_to_all(pieces, "tp", 0, 0, tiled=True).astype(f32).sum(axis=0)


def half_back(u, c, z, tp, gate_up, down):
    field = u.astype(f32)
    scale = lax.rsqrt(jnp.mean(field * field, axis=1, keepdims=True) + eps)
    normed_b = (field * scale).astype(bf16)
    both = contract(normed_b, z, gate_up)
    n = both.shape[1] // 2
    gate, upper = both[:, :n], both[:, n:]
    back = 0.5 * contract(c, z, down)
    logistic = jax.nn.sigmoid(gate)
    activated = gate * logistic
    hidden = (activated * upper).astype(bf16)
    d_gate = (back * upper * logistic * (1.0 + gate * (1.0 - logistic))).astype(bf16)
    d_up = (back * activated).astype(bf16)
    partial = spread(jnp.concatenate([d_gate, d_up], axis=1), z, gate_up)
    rows = u.shape[0] // lax.axis_size("tp")
    d_normed = own_rows(partial)
    field = lax.dynamic_slice_in_dim(u, tp * rows, rows, axis=0).astype(f32)
    scale = lax.rsqrt(jnp.mean(field * field, axis=1, keepdims=True) + eps)
    normed = field * scale
    carried = lax.dynamic_slice_in_dim(c, tp * rows, rows, axis=0).astype(f32)
    d_field = carried + scale * (
        d_normed - normed * jnp.mean(d_normed * normed, axis=1, keepdims=True)
    )
    return from_everyone(d_field.astype(bf16), "tp").reshape(u.shape), hidden


def down_share(hidden, grad, z):
    span = grad.shape[1] // 4
    half = span // 2

    def part(m):
        cols = lax.dynamic_slice_in_dim(grad, ((z + m) % 4) * span, span, axis=1)
        return 0.5 * lax.dot_general(
            cols, hidden, (((0,), (0,)), ((), ())), preferred_element_type=f32
        )

    far = part(2).astype(bf16)
    top = take_from(far[:half], Z, -2).astype(f32)
    bottom = take_from(far[half:], Z, 2).astype(f32)
    next_ = take_from(part(1).astype(bf16), Z, -1).astype(f32)
    last = take_from(part(3).astype(bf16), Z, 1).astype(f32)
    column = part(0) + next_ + last + jnp.concatenate([top, bottom], axis=0)
    column = column.astype(bf16).reshape(lax.axis_size("fs_1"), -1, hidden.shape[1])
    share = lax.all_to_all(column, "fs_1", 0, 0, tiled=True).astype(f32).sum(axis=0)
    share = share.astype(bf16)
    return share.astype(f32) + take_from(share, "rep", 1).astype(f32)


def on_device(
    tokens,
    mid_tokens,
    out_grad,
    gate_first,
    up_first,
    down_first,
    gate_second,
    up_second,
    down_second,
):
    z = lax.axis_index("fs_0")
    tp = lax.axis_index("tp")
    gu2 = along_y(jnp.concatenate([gate_second, up_second], axis=1))
    dn2 = along_y(after(down_second.T, gu2))
    gu1 = along_y(after(jnp.concatenate([gate_first, up_first], axis=1), dn2))
    dn1 = along_y(after(down_first.T, gu1))
    gate_up_2 = along_z(gu2)
    down_2 = along_z(after(dn2, gate_up_2[1][2], gate_up_2[2][2]))
    gate_up_1 = along_z(after(gu1, down_2[1][2], down_2[2][2]))
    down_1 = along_z(after(dn1, gate_up_1[1][2], gate_up_1[2][2]))
    mid_grad, _ = half_back(mid_tokens, out_grad, z, tp, gate_up_2, down_2)
    input_grad, hidden = half_back(tokens, mid_grad, z, tp, gate_up_1, down_1)
    share = down_share(hidden, mid_grad, z)
    norms = from_everyone(jnp.sum(share * share, axis=0), FS).sum(axis=0)
    return (input_grad, share.T, norms)


def solution(mesh):
    torus = Mesh(
        mesh.devices.reshape(mesh.shape["rep"], 4, 8, mesh.shape["tp"]),
        ("rep", "fs_0", "fs_1", "tp"),
    )
    placed = (
        P(REP_FS, None),
        P(REP_FS, None),
        P(REP_FS, None),
        P(FS, "tp"),
        P(FS, "tp"),
        P("tp", FS),
        P(FS, "tp"),
        P(FS, "tp"),
        P("tp", FS),
    )
    return jax.shard_map(
        on_device,
        mesh=torus,
        in_specs=placed,
        out_specs=(P(REP_FS, None), P("tp", FS), P("tp")),
        check_vma=False,
    )
```

```python
import jax
import jax.numpy as jnp
from jax import lax
from jax.experimental import pallas as pl
from jax.experimental.pallas import tpu as pltpu
from jax.sharding import Mesh
from jax.sharding import PartitionSpec as P


FS = ("fs_0", "fs_1")
Z = ("rep", "fs_0")
REP_FS = ("rep", "fs_0", "fs_1")
f32 = jnp.float32
bf16 = jnp.bfloat16

eps = 1e-06
PIECES = ((0, None), (1, None), (3, None), (2, 0), (2, 1))
ROWS_ROWS = (((1,), (1,)), ((), ()))


def take_from(value, axis, step):
    n = lax.axis_size(axis)
    return lax.ppermute(value, axis, [((i + step) % n, i) for i in range(n)])


def from_everyone(value, axis):
    n = lax.axis_size(axis)
    return lax.all_to_all(
        jnp.broadcast_to(value[None], (n, *value.shape)), axis, 0, 0, tiled=True
    )


def along_y(value):
    whole = from_everyone(value, "fs_1")
    return whole.reshape(-1, value.shape[1])


def along_z(value):
    half = value.shape[0] // 2
    next_ = take_from(value, Z, 1)
    last = take_from(value, Z, -1)
    top = take_from(next_[:half], Z, 1)
    bottom = take_from(last[half:], Z, -1)
    return (value, next_, last, top, bottom)


def after(value, *others):
    return lax.optimization_barrier((value, *others))[0]


def span_of(z, piece, width):
    m, half = piece
    quarter = width // 4
    start = lax.rem(z + m, 4) * quarter
    if half is None:
        return pl.ds(pl.multiple_of(start, quarter), quarter)
    return pl.ds(pl.multiple_of(start + half * (quarter // 2), quarter // 2), quarter // 2)


def forward_body(z_ref, u_ref, w0, w1, w2, w3, w4, both_ref, hidden_ref):
    z = z_ref[0]
    width = u_ref.shape[1]
    field = u_ref[...].astype(f32)
    scale = lax.rsqrt(jnp.mean(field * field, axis=1, keepdims=True) + eps)
    total = None
    for piece, w in zip(PIECES, (w0, w1, w2, w3, w4)):
        normed_b = (u_ref[:, span_of(z, piece, width)].astype(f32) * scale).astype(bf16)
        part = jnp.dot(normed_b, w[...], preferred_element_type=f32)
        total = part if total is None else total + part
    both_ref[...] = total
    n = total.shape[1] // 2
    gate, upper = total[:, :n], total[:, n:]
    hidden_ref[...] = (gate * jax.nn.sigmoid(gate) * upper).astype(bf16)


def backward_body(z_ref, c_ref, both_ref, d0, d1, d2, d3, d4, w0, w1, w2, w3, w4, out_ref):
    z = z_ref[0]
    width = c_ref.shape[1]
    total = None
    for piece, w in zip(PIECES, (d0, d1, d2, d3, d4)):
        part = jnp.dot(
            c_ref[:, span_of(z, piece, width)], w[...], preferred_element_type=f32
        )
        total = part if total is None else total + part
    back = 0.5 * total
    n = back.shape[1]
    gate, upper = both_ref[:, :n], both_ref[:, n:]
    logistic = jax.nn.sigmoid(gate)
    d_gate = (back * upper * logistic * (1.0 + gate * (1.0 - logistic))).astype(bf16)
    d_up = (back * (gate * logistic)).astype(bf16)
    d_both = jnp.concatenate([d_gate, d_up], axis=1)
    for piece, w in zip(PIECES, (w0, w1, w2, w3, w4)):
        part = lax.dot_general(d_both, w[...], ROWS_ROWS, preferred_element_type=f32)
        out_ref[:, span_of(z, piece, width)] = part.astype(bf16)


SMEM = pl.BlockSpec(memory_space=pltpu.SMEM)
VMEM = pl.BlockSpec(memory_space=pltpu.VMEM)


def forward(z, u, gate_up):
    tokens, n = u.shape[0], gate_up[0].shape[1]
    return pl.pallas_call(
        forward_body,
        in_specs=[SMEM] + [VMEM] * 6,
        out_specs=(VMEM, VMEM),
        out_shape=(
            jax.ShapeDtypeStruct((tokens, n), f32),
            jax.ShapeDtypeStruct((tokens, n // 2), bf16),
        ),
        cost_estimate=pl.CostEstimate(
            flops=2 * tokens * u.shape[1] * n, bytes_accessed=5 << 20, transcendentals=0
        ),
    )(z, u, *gate_up)


def backward(z, c, both, down, gate_up):
    return pl.pallas_call(
        backward_body,
        in_specs=[SMEM] + [VMEM] * 12,
        out_specs=VMEM,
        out_shape=jax.ShapeDtypeStruct(c.shape, bf16),
        cost_estimate=pl.CostEstimate(
            flops=3 * c.shape[0] * c.shape[1] * both.shape[1],
            bytes_accessed=8 << 20,
            transcendentals=0,
        ),
    )(z, c, both, *down, *gate_up)


def own_rows(partial, u, c, tp):
    n = lax.axis_size("tp")
    pieces = partial.reshape(n, -1, partial.shape[1])
    pieces = lax.all_to_all(pieces, "tp", 0, 0, tiled=True)
    d_normed = pieces.astype(f32).sum(axis=0)
    rows = u.shape[0] // n
    field = lax.dynamic_slice_in_dim(u, tp * rows, rows, axis=0).astype(f32)
    scale = lax.rsqrt(jnp.mean(field * field, axis=1, keepdims=True) + eps)
    normed = field * scale
    carried = lax.dynamic_slice_in_dim(c, tp * rows, rows, axis=0).astype(f32)
    d_field = carried + scale * (
        d_normed - normed * jnp.mean(d_normed * normed, axis=1, keepdims=True)
    )
    return d_field.astype(bf16)


def all_rows(value, tp):
    n = lax.axis_size("tp")
    rows = value.shape[0]
    core, x = tp % 2, tp // 2
    quarters = [value]
    for j in (1, 2, 3):
        quarters.append(lax.ppermute(value, "tp", [((i + 2 * j) % n, i) for i in range(n)]))
    mine = jnp.stack(quarters)
    other = lax.ppermute(mine, "tp", [(i, i ^ 1) for i in range(n)])
    pair = jnp.where(core == 0, jnp.stack([mine, other], 1), jnp.stack([other, mine], 1))
    return jnp.roll(pair, x, axis=0).reshape(n * rows, -1)


def down_column(hidden, grad, z):
    span = grad.shape[1] // 4
    half = span // 2

    def part(m):
        cols = lax.dynamic_slice_in_dim(grad, ((z + m) % 4) * span, span, axis=1)
        return 0.5 * lax.dot_general(
            cols, hidden, (((0,), (0,)), ((), ())), preferred_element_type=f32
        )

    far = part(2).astype(bf16)
    top = take_from(far[:half], Z, -2).astype(f32)
    bottom = take_from(far[half:], Z, 2).astype(f32)
    next_ = take_from(part(1).astype(bf16), Z, -1).astype(f32)
    last = take_from(part(3).astype(bf16), Z, 1).astype(f32)
    column = part(0) + next_ + last + jnp.concatenate([top, bottom], axis=0)
    return column.astype(bf16).reshape(lax.axis_size("fs_1"), -1, hidden.shape[1])


def step(
    tokens,
    mid_tokens,
    out_grad,
    gate_first,
    up_first,
    down_first,
    gate_second,
    up_second,
    down_second,
):
    z = lax.axis_index("fs_0")
    zs = z.astype(jnp.int32).reshape(1)
    tp = lax.axis_index("tp")

    gu2 = along_y(jnp.concatenate([gate_second, up_second], axis=1))
    dn2 = along_y(after(down_second.T, gu2))
    gu1 = along_y(after(jnp.concatenate([gate_first, up_first], axis=1), dn2))
    dn1 = along_y(after(down_first.T, gu1))
    gate_up_2 = along_z(gu2)
    down_2 = along_z(after(dn2, gate_up_2[1], gate_up_2[2]))
    both_2, _ = forward(zs, mid_tokens, gate_up_2)
    partial_2 = backward(zs, out_grad, both_2, down_2, gate_up_2)

    gate_up_1 = along_z(after(gu1, down_2[1], down_2[2]))
    down_1 = along_z(after(dn1, gate_up_1[1], gate_up_1[2]))
    rows_2 = own_rows(after(partial_2, dn1), mid_tokens, out_grad, tp)
    mid_grad = from_everyone(rows_2, "tp").reshape(mid_tokens.shape)

    both_1, hidden = forward(zs, tokens, gate_up_1)
    column = down_column(hidden, mid_grad, z)
    partial_1 = backward(zs, mid_grad, both_1, down_1, gate_up_1)
    rows_1 = own_rows(partial_1, tokens, mid_grad, tp)
    column = after(column, rows_1)
    share = lax.all_to_all(column, "fs_1", 0, 0, tiled=True)
    share = share.astype(f32).sum(axis=0).astype(bf16)
    input_grad = all_rows(rows_1, tp)
    share = share.astype(f32) + take_from(share, "rep", 1).astype(f32)
    norms = from_everyone(jnp.sum(share * share, axis=0), FS).sum(axis=0)
    return (input_grad, share.T, norms)


def solution(mesh):
    torus = Mesh(
        mesh.devices.reshape(mesh.shape["rep"], 4, 8, mesh.shape["tp"]),
        ("rep", "fs_0", "fs_1", "tp"),
    )
    placed = (
        P(REP_FS, None),
        P(REP_FS, None),
        P(REP_FS, None),
        P(FS, "tp"),
        P(FS, "tp"),
        P("tp", FS),
        P(FS, "tp"),
        P(FS, "tp"),
        P("tp", FS),
    )
    return jax.shard_map(
        step,
        mesh=torus,
        in_specs=placed,
        out_specs=(P(REP_FS, None), P("tp", FS), P("tp")),
        check_vma=False,
    )
```

```python
import jax
import jax.numpy as jnp
from jax import lax
from jax.experimental import pallas as pl
from jax.experimental.pallas import tpu as pltpu
from jax.sharding import Mesh
from jax.sharding import PartitionSpec as P


FS = ("fs_0", "fs_1")
Z = ("rep", "fs_0")
REP_FS = ("rep", "fs_0", "fs_1")
f32 = jnp.float32
bf16 = jnp.bfloat16

eps = 1e-06
PIECES = ((0, None), (1, None), (3, None), (2, 0), (2, 1))
ROWS_ROWS = (((1,), (1,)), ((), ()))


def take_from(value, axis, step):
    n = lax.axis_size(axis)
    return lax.ppermute(value, axis, [((i + step) % n, i) for i in range(n)])


def from_everyone(value, axis):
    n = lax.axis_size(axis)
    return lax.all_to_all(
        jnp.broadcast_to(value[None], (n, *value.shape)), axis, 0, 0, tiled=True
    )


def along_y(value):
    whole = from_everyone(value, "fs_1")
    return whole.reshape(-1, value.shape[1])


def along_z(value):
    half = value.shape[0] // 2
    next_ = take_from(value, Z, 1)
    last = take_from(value, Z, -1)
    top = take_from(next_[:half], Z, 1)
    bottom = take_from(last[half:], Z, -1)
    return (value, next_, last, top, bottom)


def after(value, *others):
    return lax.optimization_barrier((value, *others))[0]


def span_of(z, piece, width):
    m, half = piece
    quarter = width // 4
    start = lax.rem(z + m, 4) * quarter
    if half is None:
        return pl.ds(pl.multiple_of(start, quarter), quarter)
    return pl.ds(pl.multiple_of(start + half * (quarter // 2), quarter // 2), quarter // 2)


def gate_up_of(z, u_ref, pieces, n):
    width = u_ref.shape[1]
    field = u_ref[...].astype(f32)
    scale = lax.rsqrt(jnp.mean(field * field, axis=1, keepdims=True) + eps)
    total = None
    for piece, w in zip(PIECES, pieces):
        normed_b = (u_ref[:, span_of(z, piece, width)].astype(f32) * scale).astype(bf16)
        part = jnp.dot(normed_b, w[:, : 2 * n], preferred_element_type=f32)
        total = part if total is None else total + part
    return total[:, :n], total[:, n:]


def partial_of(z, c_ref, gate, upper, pieces, out_ref):
    width, n = c_ref.shape[1], gate.shape[1]
    total = None
    for piece, w in zip(PIECES, pieces):
        part = jnp.dot(
            c_ref[:, span_of(z, piece, width)], w[:, 2 * n :], preferred_element_type=f32
        )
        total = part if total is None else total + part
    back = 0.5 * total
    logistic = jax.nn.sigmoid(gate)
    d_gate = (back * upper * logistic * (1.0 + gate * (1.0 - logistic))).astype(bf16)
    d_up = (back * (gate * logistic)).astype(bf16)
    d_both = jnp.concatenate([d_gate, d_up], axis=1)
    for piece, w in zip(PIECES, pieces):
        part = lax.dot_general(d_both, w[:, : 2 * n], ROWS_ROWS, preferred_element_type=f32)
        out_ref[:, span_of(z, piece, width)] = part.astype(bf16)


def block_body(z_ref, u_ref, c_ref, w0, w1, w2, w3, w4, out_ref):
    z, pieces = z_ref[0], (w0, w1, w2, w3, w4)
    gate, upper = gate_up_of(z, u_ref, pieces, w0.shape[1] // 3)
    partial_of(z, c_ref, gate, upper, pieces, out_ref)


def forward_body(z_ref, u_ref, w0, w1, w2, w3, w4, both_ref, hidden_ref):
    n = hidden_ref.shape[1]
    gate, upper = gate_up_of(z_ref[0], u_ref, (w0, w1, w2, w3, w4), n)
    both_ref[:, :n] = gate
    both_ref[:, n:] = upper
    hidden_ref[...] = (gate * jax.nn.sigmoid(gate) * upper).astype(bf16)


def backward_body(z_ref, c_ref, both_ref, w0, w1, w2, w3, w4, out_ref):
    n = both_ref.shape[1] // 2
    pieces = (w0, w1, w2, w3, w4)
    partial_of(z_ref[0], c_ref, both_ref[:, :n], both_ref[:, n:], pieces, out_ref)


SMEM = pl.BlockSpec(memory_space=pltpu.SMEM)
VMEM = pl.BlockSpec(memory_space=pltpu.VMEM)


def kernel(body, outs, matmuls, z, *arrays):
    tokens, width, n = arrays[0].shape[0], arrays[0].shape[1], arrays[-1].shape[1] // 3
    return pl.pallas_call(
        body,
        in_specs=[SMEM] + [VMEM] * len(arrays),
        out_specs=tuple(VMEM for _ in outs),
        out_shape=tuple(jax.ShapeDtypeStruct(*o) for o in outs),
        cost_estimate=pl.CostEstimate(
            flops=2 * tokens * width * n * matmuls, bytes_accessed=6 << 20, transcendentals=0
        ),
    )(z, *arrays)


def gradient_of_rows(d_normed, u, c, tp):
    rows = d_normed.shape[0]
    field = lax.dynamic_slice_in_dim(u, tp * rows, rows, axis=0).astype(f32)
    scale = lax.rsqrt(jnp.mean(field * field, axis=1, keepdims=True) + eps)
    normed = field * scale
    carried = lax.dynamic_slice_in_dim(c, tp * rows, rows, axis=0).astype(f32)
    d_field = carried + scale * (
        d_normed - normed * jnp.mean(d_normed * normed, axis=1, keepdims=True)
    )
    return d_field.astype(bf16)


def own_rows(partial):
    pieces = partial.reshape(lax.axis_size("tp"), -1, partial.shape[1])
    pieces = lax.all_to_all(pieces, "tp", 0, 0, tiled=True)
    return pieces.astype(f32).sum(axis=0)


def swap_cores(value):
    return lax.ppermute(value, "tp", [(i, i ^ 1) for i in range(lax.axis_size("tp"))])


def take_x(value, step):
    n = lax.axis_size("tp")
    return lax.ppermute(value, "tp", [((i + 2 * step) % n, i) for i in range(n)])


def own_rows_by_permutes(partial, core, x):
    rows = partial.shape[0]
    half, n = rows // 2, rows // 8
    other = swap_cores(lax.dynamic_slice_in_dim(partial, (1 - core) * half, half, axis=0))
    mine = lax.dynamic_slice_in_dim(partial, core * half, half, axis=0)
    chip = (mine.astype(f32) + other.astype(f32)).astype(bf16)

    def block(j):
        return lax.dynamic_slice_in_dim(chip, ((x + j) % 4) * n, n, axis=0)

    total = block(0).astype(f32)
    for j in (2, 1, 3):
        total = total + take_x(block(j), -j).astype(f32)
    return total


def all_rows(value, core, x):
    rows = value.shape[0]
    quarters = [value]
    for j in (1, 2, 3):
        quarters.append(take_x(value, j))
    mine = jnp.stack(quarters)
    other = swap_cores(mine)
    pair = jnp.where(core == 0, jnp.stack([mine, other]), jnp.stack([other, mine]))
    return jnp.roll(pair, x, axis=1).reshape(8 * rows, -1)


def step(
    tokens,
    mid_tokens,
    out_grad,
    gate_first,
    up_first,
    down_first,
    gate_second,
    up_second,
    down_second,
):
    zs = lax.axis_index("fs_0").astype(jnp.int32).reshape(1)
    tp = lax.axis_index("tp")
    core, x = tp % 2, tp // 2
    rep = lax.axis_index("rep")
    n, width = gate_first.shape[1], tokens.shape[1]
    like_u = (tokens.shape, bf16)

    all2 = along_y(jnp.concatenate([gate_second, up_second, down_second.T], axis=1))
    all1 = jnp.concatenate([gate_first, up_first, down_first.T], axis=1)
    all1 = along_y(after(all1, all2))
    weight_2 = along_z(all2)
    weight_1 = along_z(after(all1, weight_2[1], weight_2[2]))

    (partial,) = kernel(block_body, (like_u,), 5, zs, mid_tokens, out_grad, *weight_2)
    rows = own_rows(after(partial, all1))
    rows = gradient_of_rows(rows, mid_tokens, out_grad, tp)
    mid_grad = from_everyone(rows, "tp").reshape(mid_tokens.shape)

    both, hidden = kernel(
        forward_body,
        (((tokens.shape[0], 2 * n), f32), ((tokens.shape[0], n), bf16)),
        2,
        zs,
        tokens,
        *weight_1,
    )
    share = 0.5 * lax.dot_general(
        mid_grad, hidden, (((0,), (0,)), ((), ())), preferred_element_type=f32
    )
    share = share.astype(bf16).reshape(width // 64, 2, 32, n).swapaxes(0, 1)
    share = lax.all_to_all(share.reshape(width // 32, 32, n), REP_FS, 0, 0, tiled=True)
    share = share.astype(f32).sum(axis=0)
    twin = take_from(share, "rep", 1)
    norms = from_everyone(jnp.sum(share * share, axis=0), REP_FS).sum(axis=0)
    share = jnp.where(rep == 0, jnp.stack([share, twin]), jnp.stack([twin, share]))

    (partial,) = kernel(backward_body, (like_u,), 3, zs, mid_grad, both, *weight_1)
    rows = own_rows_by_permutes(partial, core, x)
    rows = gradient_of_rows(rows, tokens, mid_grad, core * 4 + x)
    input_grad = all_rows(rows, core, x)
    return (input_grad, share.reshape(64, n).T, norms)


def solution(mesh):
    torus = Mesh(
        mesh.devices.reshape(mesh.shape["rep"], 4, 8, mesh.shape["tp"]),
        ("rep", "fs_0", "fs_1", "tp"),
    )
    placed = (
        P(REP_FS, None),
        P(REP_FS, None),
        P(REP_FS, None),
        P(FS, "tp"),
        P(FS, "tp"),
        P("tp", FS),
        P(FS, "tp"),
        P(FS, "tp"),
        P("tp", FS),
    )
    return jax.shard_map(
        step,
        mesh=torus,
        in_specs=placed,
        out_specs=(P(REP_FS, None), P("tp", FS), P("tp")),
        check_vma=False,
    )
```

```python
import jax
import jax.numpy as jnp
from jax import lax
from jax.experimental import pallas as pl
from jax.experimental.pallas import tpu as pltpu
from jax.sharding import Mesh
from jax.sharding import PartitionSpec as P


FS = ("fs_0", "fs_1")
Z = ("rep", "fs_0")
REP_FS = ("rep", "fs_0", "fs_1")
FS_REP = ("fs_0", "fs_1", "rep")
f32 = jnp.float32
bf16 = jnp.bfloat16

eps = 1e-06
LEFT = 640
PIECES = (0, 1, 3, 2)
ROWS_ROWS = (((1,), (1,)), ((), ()))


def take_from(value, axis, step):
    n = lax.axis_size(axis)
    return lax.ppermute(value, axis, [((i + step) % n, i) for i in range(n)])


def from_everyone(value, axis):
    n = lax.axis_size(axis)
    return lax.all_to_all(
        jnp.broadcast_to(value[None], (n, *value.shape)), axis, 0, 0, tiled=True
    )


def along_y(value):
    whole = from_everyone(value, "fs_1")
    return whole.reshape(-1, value.shape[1])


def along_z(value, forward):
    next_ = take_from(value, Z, 1)
    last = take_from(value, Z, -1)
    far = take_from(next_ if forward > 0 else last, Z, forward)
    return (value, next_, last, far)


def after(value, *others):
    return lax.optimization_barrier((value, *others))[0]


def span_of(z, m, width):
    quarter = width // 4
    return pl.ds(pl.multiple_of(lax.rem(z + m, 4) * quarter, quarter), quarter)


def gate_up_of(z, u_ref, left, right, n):
    width = u_ref.shape[1]
    field = u_ref[...].astype(f32)
    scale = lax.rsqrt(jnp.mean(field * field, axis=1, keepdims=True) + eps)
    a = b = None
    for m, wl, wr in zip(PIECES, left, right):
        normed_b = (u_ref[:, span_of(z, m, width)].astype(f32) * scale).astype(bf16)
        part_a = jnp.dot(normed_b, wl[...], preferred_element_type=f32)
        part_b = jnp.dot(normed_b, wr[:, : 2 * n - LEFT], preferred_element_type=f32)
        a = part_a if a is None else a + part_a
        b = part_b if b is None else b + part_b
    return a[:, :n], jnp.concatenate([a[:, n:], b], axis=1)


def partial_of(z, c_ref, gate, upper, left, right, out_ref):
    width, n = c_ref.shape[1], gate.shape[1]
    total = None
    for m, wr in zip(PIECES, right):
        part = jnp.dot(
            c_ref[:, span_of(z, m, width)], wr[:, 2 * n - LEFT :], preferred_element_type=f32
        )
        total = part if total is None else total + part
    back = 0.5 * total
    logistic = jax.nn.sigmoid(gate)
    d_gate = (back * upper * logistic * (1.0 + gate * (1.0 - logistic))).astype(bf16)
    d_up = (back * (gate * logistic)).astype(bf16)
    d_left = jnp.concatenate([d_gate, d_up[:, : LEFT - n]], axis=1)
    d_right = d_up[:, LEFT - n :]
    for m, wl, wr in zip(PIECES, left, right):
        part = lax.dot_general(d_left, wl[...], ROWS_ROWS, preferred_element_type=f32)
        part = part + lax.dot_general(
            d_right, wr[:, : 2 * n - LEFT], ROWS_ROWS, preferred_element_type=f32
        )
        out_ref[:, span_of(z, m, width)] = part.astype(bf16)


def block_body(z_ref, u_ref, c_ref, *refs):
    *weight, out_ref = refs
    z, left, right = z_ref[0], weight[:4], weight[4:]
    gate, upper = gate_up_of(z, u_ref, left, right, (LEFT + right[0].shape[1]) // 3)
    partial_of(z, c_ref, gate, upper, left, right, out_ref)


def forward_body(z_ref, u_ref, *refs):
    *weight, both_ref, hidden_ref = refs
    n = hidden_ref.shape[1]
    gate, upper = gate_up_of(z_ref[0], u_ref, weight[:4], weight[4:], n)
    both_ref[:, :n] = gate
    both_ref[:, n:] = upper
    hidden_ref[...] = (gate * jax.nn.sigmoid(gate) * upper).astype(bf16)


def backward_body(z_ref, c_ref, both_ref, *refs):
    *weight, mine_ref, other_ref, out_ref = refs
    n = both_ref.shape[1] // 2
    gate, upper = both_ref[:, :n], both_ref[:, n:]
    partial_of(z_ref[0], c_ref, gate, upper, weight[:4], weight[4:], out_ref)
    core, (blocks, rows, _) = z_ref[1], mine_ref.shape
    for k in range(blocks):
        mine_ref[k] = out_ref[pl.ds(pl.multiple_of((2 * k + core) * rows, rows), rows), :]
        other_ref[k] = out_ref[pl.ds(pl.multiple_of((2 * k + 1 - core) * rows, rows), rows), :]


def gradient_of(d_normed, u, c):
    field = u.astype(f32)
    scale = lax.rsqrt(jnp.mean(field * field, axis=1, keepdims=True) + eps)
    normed = field * scale
    d_field = c.astype(f32) + scale * (
        d_normed - normed * jnp.mean(d_normed * normed, axis=1, keepdims=True)
    )
    return d_field.astype(bf16)


def spread_rows_body(tp_ref, p_ref, u_ref, c_ref, own_ref, out_ref):
    n, _, _ = p_ref.shape
    d_normed = p_ref[0].astype(f32)
    for k in range(1, n):
        d_normed = d_normed + p_ref[k].astype(f32)
    own = gradient_of(d_normed, u_ref[...], c_ref[...])
    own_ref[...] = own
    for k in range(n):
        out_ref[k] = own


def own_rows_body(tp_ref, p0, p1, p2, p3, u_ref, c_ref, own_ref):
    rows = c_ref.shape[0]
    d_normed = p0[...].astype(f32)
    for p in (p1, p2, p3):
        d_normed = d_normed + p[...].astype(f32)
    u = u_ref[pl.ds(pl.multiple_of(tp_ref[0] * rows, rows), rows), :]
    own_ref[...] = gradient_of(d_normed, u, c_ref[...])


def place_rows_body(tp_ref, q0, q1, q2, q3, other_ref, out_ref):
    rows = q0.shape[0]
    x, core = tp_ref[0] // 2, lax.rem(tp_ref[0], 2)
    for j, q in enumerate((q0, q1, q2, q3)):
        at = lax.rem(x + j, 4) * 2
        out_ref[pl.ds(pl.multiple_of((at + core) * rows, rows), rows), :] = q[...]
        out_ref[pl.ds(pl.multiple_of((at + 1 - core) * rows, rows), rows), :] = other_ref[j]


SMEM = pl.BlockSpec(memory_space=pltpu.SMEM)
VMEM = pl.BlockSpec(memory_space=pltpu.VMEM)


def kernel(body, outs, flops, scalars, *arrays, scratch=()):
    return pl.pallas_call(
        body,
        in_specs=[SMEM] + [VMEM] * len(arrays),
        out_specs=tuple(VMEM for _ in outs),
        out_shape=tuple(jax.ShapeDtypeStruct(*o) for o in outs),
        scratch_shapes=scratch,
        cost_estimate=pl.CostEstimate(
            flops=flops, bytes_accessed=6 << 20, transcendentals=0
        ),
    )(scalars, *arrays)


def own_rows(partial):
    pieces = partial.reshape(lax.axis_size("tp"), -1, partial.shape[1])
    return lax.all_to_all(pieces, "tp", 0, 0, tiled=True)


def swap_cores(value):
    return lax.ppermute(value, "tp", [(i, i ^ 1) for i in range(lax.axis_size("tp"))])


def take_x(value, step):
    n = lax.axis_size("tp")
    return lax.ppermute(value, "tp", [((i + 2 * step) % n, i) for i in range(n)])


def own_rows_by_permutes(mine, other, x):
    other = swap_cores(other)
    chip = (mine.astype(f32) + other.astype(f32)).astype(bf16)

    def block(j):
        return lax.dynamic_index_in_dim(chip, (x + j) % 4, axis=0, keepdims=False)

    pieces = [block(0)]
    for j in (2, 1, 3):
        pieces.append(take_x(block(j), -j))
    return pieces


def all_rows(value, tps):
    quarters = [value]
    for j in (1, 2, 3):
        quarters.append(take_x(value, j))
    stacked = jnp.stack(quarters)
    other = swap_cores(stacked)
    out = ((8 * value.shape[0], value.shape[1]), bf16)
    (whole,) = kernel(place_rows_body, (out,), 1 << 20, tps, *quarters, other)
    return whole


def step(
    tokens,
    mid_tokens,
    out_grad,
    gate_first,
    up_first,
    down_first,
    gate_second,
    up_second,
    down_second,
):
    tp = lax.axis_index("tp")
    tps = tp.astype(jnp.int32).reshape(1)
    zs = jnp.stack([lax.axis_index("fs_0"), tp % 2]).astype(jnp.int32)
    n, width = gate_first.shape[1], tokens.shape[1]
    like_u = (tokens.shape, bf16)

    flops = 2 * tokens.shape[0] * width * n

    def parts(whole):
        return whole[:, :LEFT], whole[:, LEFT:]

    y2 = along_y(jnp.concatenate([gate_second, up_second, down_second.T], axis=1))
    y1 = jnp.concatenate([gate_first, up_first, down_first.T], axis=1)
    y1 = along_y(after(y1, y2))
    a2, b2 = parts(y2)
    a1, b1 = parts(y1)
    a2 = along_z(a2, 1)
    b2 = along_z(b2, -1)
    a1 = along_z(a1, 1)
    b1 = along_z(b1, -1)

    (partial,) = kernel(block_body, (like_u,), 5 * flops, zs, mid_tokens, out_grad, *a2, *b2)
    pieces = own_rows(partial)
    rows, like_rows = pieces.shape[1], (pieces.shape[1:], bf16)
    mid_rows, spread = kernel(
        spread_rows_body,
        (like_rows, (pieces.shape, bf16)),
        1 << 24,
        tps,
        pieces,
        lax.dynamic_slice_in_dim(mid_tokens, tp * rows, rows, axis=0),
        lax.dynamic_slice_in_dim(out_grad, tp * rows, rows, axis=0),
    )
    mid_grad = lax.all_to_all(spread, "tp", 0, 0, tiled=True).reshape(mid_tokens.shape)

    both, hidden = kernel(
        forward_body,
        (((tokens.shape[0], 2 * n), f32), ((tokens.shape[0], n), bf16)),
        2 * flops,
        zs,
        tokens,
        *a1,
        *b1,
    )
    share = 0.5 * lax.dot_general(
        mid_grad, hidden, (((0,), (0,)), ((), ())), preferred_element_type=f32
    )
    share = share.astype(bf16).reshape(lax.axis_size(FS_REP), -1, n)
    share = lax.all_to_all(share, FS_REP, 0, 0, tiled=True)
    share = share.astype(f32).sum(axis=0)
    twin = take_from(share, "rep", 1)
    norms = from_everyone(jnp.sum(share * share, axis=0), FS_REP).sum(axis=0)
    first = lax.axis_index("rep") == 0
    share = jnp.where(first, jnp.stack([share, twin]), jnp.stack([twin, share]))

    half = ((4, rows, width), bf16)
    mine, other = kernel(
        backward_body,
        (half, half),
        3 * flops,
        zs,
        mid_grad,
        both,
        *a1,
        *b1,
        scratch=[pltpu.VMEM(tokens.shape, bf16)],
    )
    pieces = own_rows_by_permutes(mine, other, tp // 2)
    (in_rows,) = kernel(own_rows_body, (like_rows,), 1 << 24, tps, *pieces, tokens, mid_rows)
    input_grad = all_rows(in_rows, tps)
    return (input_grad, share.reshape(-1, n).T, norms)


def solution(mesh):
    torus = Mesh(
        mesh.devices.reshape(mesh.shape["rep"], 4, 8, mesh.shape["tp"]),
        ("rep", "fs_0", "fs_1", "tp"),
    )
    placed = (
        P(REP_FS, None),
        P(REP_FS, None),
        P(REP_FS, None),
        P(FS, "tp"),
        P(FS, "tp"),
        P("tp", FS),
        P(FS, "tp"),
        P(FS, "tp"),
        P("tp", FS),
    )
    return jax.shard_map(
        step,
        mesh=torus,
        in_specs=placed,
        out_specs=(P(REP_FS, None), P("tp", FS), P("tp")),
        check_vma=False,
    )
```

```python
import jax
import jax.numpy as jnp
from jax import lax
from jax.experimental import pallas as pl
from jax.experimental.pallas import tpu as pltpu
from jax.sharding import Mesh
from jax.sharding import PartitionSpec as P


FS = ("fs_0", "fs_1")
Z = ("rep", "fs_0")
REP_FS = ("rep", "fs_0", "fs_1")
FS_REP = ("fs_0", "fs_1", "rep")
f32 = jnp.float32
bf16 = jnp.bfloat16

eps = 1e-06
LEFT = 640
PIECES = (0, 1, 3, 2)
ROWS_ROWS = (((1,), (1,)), ((), ()))


def take_from(value, axis, step):
    n = lax.axis_size(axis)
    return lax.ppermute(value, axis, [((i + step) % n, i) for i in range(n)])


def from_everyone(value, axis):
    n = lax.axis_size(axis)
    return lax.all_to_all(
        jnp.broadcast_to(value[None], (n, *value.shape)), axis, 0, 0, tiled=True
    )


def along_y(value):
    whole = from_everyone(value, "fs_1")
    return whole.reshape(-1, value.shape[1])


def along_z(value, forward):
    next_ = take_from(value, Z, 1)
    last = take_from(value, Z, -1)
    far = take_from(next_ if forward > 0 else last, Z, forward)
    return (value, next_, last, far)


def after(value, *others):
    return lax.optimization_barrier((value, *others))[0]


def span_of(z, m, width):
    quarter = width // 4
    return pl.ds(pl.multiple_of(lax.rem(z + m, 4) * quarter, quarter), quarter)


def scale_of(u_ref):
    field = u_ref[...].astype(f32)
    return lax.rsqrt(jnp.mean(field * field, axis=1, keepdims=True) + eps)


def gate_up_of(z, u_ref, scale, places, left, right, n):
    width = u_ref.shape[1]
    a = b = None
    for m, wl, wr in zip(places, left, right):
        normed_b = (u_ref[:, span_of(z, m, width)].astype(f32) * scale).astype(bf16)
        part_a = jnp.dot(normed_b, wl[...], preferred_element_type=f32)
        part_b = jnp.dot(normed_b, wr[:, : 2 * n - LEFT], preferred_element_type=f32)
        a = part_a if a is None else a + part_a
        b = part_b if b is None else b + part_b
    return a, b


def back_of(z, c_ref, places, right, n):
    width = c_ref.shape[1]
    total = None
    for m, wr in zip(places, right):
        part = jnp.dot(
            c_ref[:, span_of(z, m, width)], wr[:, 2 * n - LEFT :], preferred_element_type=f32
        )
        total = part if total is None else total + part
    return total


def partial_of(z, back, gate, upper, left, right, out_ref):
    width, n = out_ref.shape[1], gate.shape[1]
    back = 0.5 * back
    logistic = jax.nn.sigmoid(gate)
    d_gate = (back * upper * logistic * (1.0 + gate * (1.0 - logistic))).astype(bf16)
    d_up = (back * (gate * logistic)).astype(bf16)
    d_left = jnp.concatenate([d_gate, d_up[:, : LEFT - n]], axis=1)
    d_right = d_up[:, LEFT - n :]
    for m, wl, wr in zip(PIECES, left, right):
        part = lax.dot_general(d_left, wl[...], ROWS_ROWS, preferred_element_type=f32)
        part = part + lax.dot_general(
            d_right, wr[:, : 2 * n - LEFT], ROWS_ROWS, preferred_element_type=f32
        )
        out_ref[:, span_of(z, m, width)] = part.astype(bf16)


def near_body(z_ref, u_ref, c_ref, *refs):
    *weight, sums_ref, scale_ref = refs
    z, left, right = z_ref[0], weight[:3], weight[3:]
    n = sums_ref.shape[1] // 3
    scale = scale_of(u_ref)
    a, b = gate_up_of(z, u_ref, scale, PIECES[:3], left, right, n)
    sums_ref[:, :LEFT] = a
    sums_ref[:, LEFT : 2 * n] = b
    sums_ref[:, 2 * n :] = back_of(z, c_ref, PIECES[:3], right, n)
    scale_ref[...] = jnp.broadcast_to(scale, scale_ref.shape)


def block_body(z_ref, u_ref, c_ref, sums_ref, scale_ref, *refs):
    *weight, out_ref = refs
    z, left, right = z_ref[0], weight[:4], weight[4:]
    n = sums_ref.shape[1] // 3
    a, b = gate_up_of(z, u_ref, scale_ref[:, :1], PIECES[3:], left[3:], right[3:], n)
    a, b = a + sums_ref[:, :LEFT], b + sums_ref[:, LEFT : 2 * n]
    back = back_of(z, c_ref, PIECES[3:], right[3:], n) + sums_ref[:, 2 * n :]
    upper = jnp.concatenate([a[:, n:], b], axis=1)
    partial_of(z, back, a[:, :n], upper, left, right, out_ref)


def near_forward_body(z_ref, u_ref, *refs):
    *weight, sums_ref, scale_ref = refs
    scale = scale_of(u_ref)
    n = sums_ref.shape[1] // 2
    a, b = gate_up_of(z_ref[0], u_ref, scale, PIECES[:3], weight[:3], weight[3:], n)
    sums_ref[:, :LEFT] = a
    sums_ref[:, LEFT:] = b
    scale_ref[...] = jnp.broadcast_to(scale, scale_ref.shape)


def forward_body(z_ref, u_ref, sums_ref, scale_ref, left_ref, right_ref, both_ref, hidden_ref):
    n = hidden_ref.shape[1]
    scale = scale_ref[:, :1]
    a, b = gate_up_of(z_ref[0], u_ref, scale, PIECES[3:], [left_ref], [right_ref], n)
    total = jnp.concatenate([a, b], axis=1) + sums_ref[...]
    gate, upper = total[:, :n], total[:, n:]
    both_ref[...] = total
    hidden_ref[...] = (gate * jax.nn.sigmoid(gate) * upper).astype(bf16)


def backward_body(z_ref, c_ref, both_ref, *refs):
    *weight, mine_ref, other_ref, out_ref = refs
    n = both_ref.shape[1] // 2
    gate, upper = both_ref[:, :n], both_ref[:, n:]
    back = back_of(z_ref[0], c_ref, PIECES, weight[4:], n)
    partial_of(z_ref[0], back, gate, upper, weight[:4], weight[4:], out_ref)
    core, (blocks, rows, _) = z_ref[1], mine_ref.shape
    for k in range(blocks):
        mine_ref[k] = out_ref[pl.ds(pl.multiple_of((2 * k + core) * rows, rows), rows), :]
        other_ref[k] = out_ref[pl.ds(pl.multiple_of((2 * k + 1 - core) * rows, rows), rows), :]


def gradient_of(d_normed, u, c):
    field = u.astype(f32)
    scale = lax.rsqrt(jnp.mean(field * field, axis=1, keepdims=True) + eps)
    normed = field * scale
    d_field = c.astype(f32) + scale * (
        d_normed - normed * jnp.mean(d_normed * normed, axis=1, keepdims=True)
    )
    return d_field.astype(bf16)


def spread_rows_body(tp_ref, p_ref, u_ref, c_ref, own_ref, out_ref):
    n, _, _ = p_ref.shape
    d_normed = p_ref[0].astype(f32)
    for k in range(1, n):
        d_normed = d_normed + p_ref[k].astype(f32)
    own = gradient_of(d_normed, u_ref[...], c_ref[...])
    own_ref[...] = own
    for k in range(n):
        out_ref[k] = own


def own_rows_body(tp_ref, p0, p1, p2, p3, u_ref, c_ref, own_ref):
    rows = c_ref.shape[0]
    d_normed = p0[...].astype(f32)
    for p in (p1, p2, p3):
        d_normed = d_normed + p[...].astype(f32)
    u = u_ref[pl.ds(pl.multiple_of(tp_ref[0] * rows, rows), rows), :]
    own_ref[...] = gradient_of(d_normed, u, c_ref[...])


def place_rows_body(tp_ref, q0, q1, q2, q3, other_ref, out_ref):
    rows = q0.shape[0]
    x, core = tp_ref[0] // 2, lax.rem(tp_ref[0], 2)
    for j, q in enumerate((q0, q1, q2, q3)):
        at = lax.rem(x + j, 4) * 2
        out_ref[pl.ds(pl.multiple_of((at + core) * rows, rows), rows), :] = q[...]
        out_ref[pl.ds(pl.multiple_of((at + 1 - core) * rows, rows), rows), :] = other_ref[j]


SMEM = pl.BlockSpec(memory_space=pltpu.SMEM)
VMEM = pl.BlockSpec(memory_space=pltpu.VMEM)


def kernel(body, outs, flops, scalars, *arrays, scratch=(), near=()):
    arrays = [
        pltpu.with_memory_space_constraint(a, pltpu.MemorySpace.VMEM) if i in near else a
        for i, a in enumerate(arrays)
    ]
    return pl.pallas_call(
        body,
        in_specs=[SMEM] + [VMEM] * len(arrays),
        out_specs=tuple(VMEM for _ in outs),
        out_shape=tuple(jax.ShapeDtypeStruct(*o) for o in outs),
        scratch_shapes=scratch,
        cost_estimate=pl.CostEstimate(
            flops=flops, bytes_accessed=6 << 20, transcendentals=0
        ),
    )(scalars, *arrays)


def own_rows(partial):
    pieces = partial.reshape(lax.axis_size("tp"), -1, partial.shape[1])
    return lax.all_to_all(pieces, "tp", 0, 0, tiled=True)


def swap_cores(value):
    return lax.ppermute(value, "tp", [(i, i ^ 1) for i in range(lax.axis_size("tp"))])


def take_x(value, step):
    n = lax.axis_size("tp")
    return lax.ppermute(value, "tp", [((i + 2 * step) % n, i) for i in range(n)])


def own_rows_by_permutes(mine, other, x):
    other = swap_cores(other)
    chip = (mine.astype(f32) + other.astype(f32)).astype(bf16)

    def block(j):
        return lax.dynamic_index_in_dim(chip, (x + j) % 4, axis=0, keepdims=False)

    pieces = [block(0)]
    for j in (2, 1, 3):
        pieces.append(take_x(block(j), -j))
    return pieces


def all_rows(value, tps):
    quarters = [value]
    for j in (1, 2, 3):
        quarters.append(take_x(value, j))
    stacked = jnp.stack(quarters)
    other = swap_cores(stacked)
    out = ((8 * value.shape[0], value.shape[1]), bf16)
    (whole,) = kernel(place_rows_body, (out,), 1 << 20, tps, *quarters, other, near=range(5))
    return whole


def step(
    tokens,
    mid_tokens,
    out_grad,
    gate_first,
    up_first,
    down_first,
    gate_second,
    up_second,
    down_second,
):
    tp = lax.axis_index("tp")
    tps = tp.astype(jnp.int32).reshape(1)
    zs = jnp.stack([lax.axis_index("fs_0"), tp % 2]).astype(jnp.int32)
    n, width = gate_first.shape[1], tokens.shape[1]
    like_u = (tokens.shape, bf16)

    flops = 2 * tokens.shape[0] * width * n

    def parts(whole):
        return whole[:, :LEFT], whole[:, LEFT:]

    y2 = along_y(jnp.concatenate([gate_second, up_second, down_second.T], axis=1))
    y1 = jnp.concatenate([gate_first, up_first, down_first.T], axis=1)
    y1 = along_y(after(y1, y2))
    a2, b2 = parts(y2)
    a1, b1 = parts(y1)
    a2 = along_z(a2, 1)
    b2 = along_z(b2, -1)
    a1 = along_z(a1, 1)
    b1 = along_z(b1, -1)

    sums, scale = kernel(
        near_body,
        (((tokens.shape[0], 3 * n), f32), ((tokens.shape[0], 128), f32)),
        2 * flops,
        zs,
        mid_tokens,
        out_grad,
        *a2[:3],
        *b2[:3],
    )
    (partial,) = kernel(
        block_body, (like_u,), 3 * flops, zs, mid_tokens, out_grad, sums, scale, *a2, *b2
    )
    pieces = own_rows(partial)
    rows, like_rows = pieces.shape[1], (pieces.shape[1:], bf16)
    mid_rows, spread = kernel(
        spread_rows_body,
        (like_rows, (pieces.shape, bf16)),
        1 << 24,
        tps,
        pieces,
        lax.dynamic_slice_in_dim(mid_tokens, tp * rows, rows, axis=0),
        lax.dynamic_slice_in_dim(out_grad, tp * rows, rows, axis=0),
        near=(0,),
    )
    mid_grad = lax.all_to_all(spread, "tp", 0, 0, tiled=True).reshape(mid_tokens.shape)

    sums_1, scale_1 = kernel(
        near_forward_body,
        (((tokens.shape[0], 2 * n), f32), ((tokens.shape[0], 128), f32)),
        flops,
        zs,
        tokens,
        *a1[:3],
        *b1[:3],
    )
    both, hidden = kernel(
        forward_body,
        (((tokens.shape[0], 2 * n), f32), ((tokens.shape[0], n), bf16)),
        flops,
        zs,
        tokens,
        sums_1,
        scale_1,
        a1[3],
        b1[3],
        near=(3, 4),
    )
    share = 0.5 * lax.dot_general(
        mid_grad, hidden, (((0,), (0,)), ((), ())), preferred_element_type=f32
    )
    share = share.astype(bf16).reshape(lax.axis_size(FS_REP), -1, n)
    share = lax.all_to_all(share, FS_REP, 0, 0, tiled=True)
    share = share.astype(f32).sum(axis=0)
    twin = take_from(share, "rep", 1)
    norms = from_everyone(jnp.sum(share * share, axis=0), FS_REP)
    norms = norms.sum(axis=0)
    first = lax.axis_index("rep") == 0
    share = jnp.where(first, jnp.stack([share, twin]), jnp.stack([twin, share]))

    half = ((4, rows, width), bf16)
    mine, other = kernel(
        backward_body,
        (half, half),
        3 * flops,
        zs,
        mid_grad,
        both,
        *a1,
        *b1,
        scratch=[pltpu.VMEM(tokens.shape, bf16)],
    )
    pieces = own_rows_by_permutes(mine, other, tp // 2)
    (in_rows,) = kernel(
        own_rows_body, (like_rows,), 1 << 24, tps, *pieces, tokens, mid_rows, near=range(4)
    )
    input_grad = all_rows(in_rows, tps)
    return (input_grad, share.reshape(-1, n).T, norms)


def solution(mesh):
    torus = Mesh(
        mesh.devices.reshape(mesh.shape["rep"], 4, 8, mesh.shape["tp"]),
        ("rep", "fs_0", "fs_1", "tp"),
    )
    placed = (
        P(REP_FS, None),
        P(REP_FS, None),
        P(REP_FS, None),
        P(FS, "tp"),
        P(FS, "tp"),
        P("tp", FS),
        P(FS, "tp"),
        P(FS, "tp"),
        P("tp", FS),
    )
    return jax.shard_map(
        step,
        mesh=torus,
        in_specs=placed,
        out_specs=(P(REP_FS, None), P("tp", FS), P("tp")),
        check_vma=False,
    )
```

```python
import jax
import jax.numpy as jnp
from jax import lax
from jax.experimental import pallas as pl
from jax.experimental.pallas import tpu as pltpu
from jax.sharding import Mesh
from jax.sharding import PartitionSpec as P


FS = ("fs_0", "fs_1")
Z = ("rep", "fs_0")
REP_FS = ("rep", "fs_0", "fs_1")
FS_REP = ("fs_0", "fs_1", "rep")
f32 = jnp.float32
bf16 = jnp.bfloat16

eps = 1e-06
LEFT = 640
PIECES = (0, 1, 3, 2)
ROWS_ROWS = (((1,), (1,)), ((), ()))


def take_from(value, axis, step):
    n = lax.axis_size(axis)
    return lax.ppermute(value, axis, [((i + step) % n, i) for i in range(n)])


def from_everyone(value, axis):
    n = lax.axis_size(axis)
    return lax.all_to_all(
        jnp.broadcast_to(value[None], (n, *value.shape)), axis, 0, 0, tiled=True
    )


def along_y(copies):
    whole = lax.all_to_all(copies, "fs_1", 0, 0, tiled=True)
    return whole.reshape(-1, copies.shape[2])


def along_z(value, forward):
    next_ = take_from(value, Z, 1)
    last = take_from(value, Z, -1)
    far = take_from(next_ if forward > 0 else last, Z, forward)
    return (value, next_, last, far)


def after(value, *others):
    return lax.optimization_barrier((value, *others))[0]


def span_of(z, m, width):
    quarter = width // 4
    return pl.ds(pl.multiple_of(lax.rem(z + m, 4) * quarter, quarter), quarter)


def pack_body(_, gate_ref, up_ref, down_ref, out_ref):
    n = gate_ref.shape[1]
    for k in range(out_ref.shape[0]):
        for j, ref in enumerate((gate_ref, up_ref, down_ref)):
            out_ref[k, :, j * n : (j + 1) * n] = ref[...]


def scale_of(u_ref):
    field = u_ref[...].astype(f32)
    return lax.rsqrt(jnp.mean(field * field, axis=1, keepdims=True) + eps)


def gate_up_of(z, u_ref, scale, places, left, right, n):
    width = u_ref.shape[1]
    a = b = None
    for m, wl, wr in zip(places, left, right):
        normed_b = (u_ref[:, span_of(z, m, width)].astype(f32) * scale).astype(bf16)
        part_a = jnp.dot(normed_b, wl[...], preferred_element_type=f32)
        part_b = jnp.dot(normed_b, wr[:, : 2 * n - LEFT], preferred_element_type=f32)
        a = part_a if a is None else a + part_a
        b = part_b if b is None else b + part_b
    return a, b


def back_of(z, c_ref, places, right, n):
    width = c_ref.shape[1]
    total = None
    for m, wr in zip(places, right):
        part = jnp.dot(
            c_ref[:, span_of(z, m, width)], wr[:, 2 * n - LEFT :], preferred_element_type=f32
        )
        total = part if total is None else total + part
    return total


def partial_of(z, back, gate, upper, left, right, out_ref):
    width, n = out_ref.shape[1], gate.shape[1]
    back = 0.5 * back
    logistic = jax.nn.sigmoid(gate)
    d_gate = (back * upper * logistic * (1.0 + gate * (1.0 - logistic))).astype(bf16)
    d_up = (back * (gate * logistic)).astype(bf16)
    d_left = jnp.concatenate([d_gate, d_up[:, : LEFT - n]], axis=1)
    d_right = d_up[:, LEFT - n :]
    for m, wl, wr in zip(PIECES, left, right):
        part = lax.dot_general(d_left, wl[...], ROWS_ROWS, preferred_element_type=f32)
        part = part + lax.dot_general(
            d_right, wr[:, : 2 * n - LEFT], ROWS_ROWS, preferred_element_type=f32
        )
        out_ref[:, span_of(z, m, width)] = part.astype(bf16)


def near_body(z_ref, u_ref, c_ref, *refs):
    *weight, sums_ref, scale_ref = refs
    z, left, right = z_ref[0], weight[:3], weight[3:]
    n = sums_ref.shape[1] // 3
    scale = scale_of(u_ref)
    a, b = gate_up_of(z, u_ref, scale, PIECES[:3], left, right, n)
    sums_ref[:, :LEFT] = a
    sums_ref[:, LEFT : 2 * n] = b
    sums_ref[:, 2 * n :] = back_of(z, c_ref, PIECES[:3], right, n)
    scale_ref[...] = jnp.broadcast_to(scale, scale_ref.shape)


def block_body(z_ref, u_ref, c_ref, sums_ref, scale_ref, *refs):
    *weight, out_ref = refs
    z, left, right = z_ref[0], weight[:4], weight[4:]
    n = sums_ref.shape[1] // 3
    a, b = gate_up_of(z, u_ref, scale_ref[:, :1], PIECES[3:], left[3:], right[3:], n)
    a, b = a + sums_ref[:, :LEFT], b + sums_ref[:, LEFT : 2 * n]
    back = back_of(z, c_ref, PIECES[3:], right[3:], n) + sums_ref[:, 2 * n :]
    upper = jnp.concatenate([a[:, n:], b], axis=1)
    partial_of(z, back, a[:, :n], upper, left, right, out_ref)


def near_forward_body(z_ref, u_ref, *refs):
    *weight, sums_ref, scale_ref = refs
    scale = scale_of(u_ref)
    n = sums_ref.shape[1] // 2
    a, b = gate_up_of(z_ref[0], u_ref, scale, PIECES[:3], weight[:3], weight[3:], n)
    sums_ref[:, :LEFT] = a
    sums_ref[:, LEFT:] = b
    scale_ref[...] = jnp.broadcast_to(scale, scale_ref.shape)


def forward_body(z_ref, u_ref, sums_ref, scale_ref, left_ref, right_ref, both_ref, hidden_ref):
    n = hidden_ref.shape[1]
    scale = scale_ref[:, :1]
    a, b = gate_up_of(z_ref[0], u_ref, scale, PIECES[3:], [left_ref], [right_ref], n)
    total = jnp.concatenate([a, b], axis=1) + sums_ref[...]
    gate, upper = total[:, :n], total[:, n:]
    both_ref[...] = total
    hidden_ref[...] = (gate * jax.nn.sigmoid(gate) * upper).astype(bf16)


def backward_body(z_ref, c_ref, both_ref, *refs):
    *weight, mine_ref, other_ref, out_ref = refs
    n = both_ref.shape[1] // 2
    gate, upper = both_ref[:, :n], both_ref[:, n:]
    back = back_of(z_ref[0], c_ref, PIECES, weight[4:], n)
    partial_of(z_ref[0], back, gate, upper, weight[:4], weight[4:], out_ref)
    core, (blocks, rows, _) = z_ref[1], mine_ref.shape
    for k in range(blocks):
        mine_ref[k] = out_ref[pl.ds(pl.multiple_of((2 * k + core) * rows, rows), rows), :]
        other_ref[k] = out_ref[pl.ds(pl.multiple_of((2 * k + 1 - core) * rows, rows), rows), :]


def gradient_of(d_normed, u, c):
    field = u.astype(f32)
    scale = lax.rsqrt(jnp.mean(field * field, axis=1, keepdims=True) + eps)
    normed = field * scale
    d_field = c.astype(f32) + scale * (
        d_normed - normed * jnp.mean(d_normed * normed, axis=1, keepdims=True)
    )
    return d_field.astype(bf16)


def spread_rows_body(tp_ref, p_ref, u_ref, c_ref, own_ref, out_ref):
    n, _, _ = p_ref.shape
    d_normed = p_ref[0].astype(f32)
    for k in range(1, n):
        d_normed = d_normed + p_ref[k].astype(f32)
    own = gradient_of(d_normed, u_ref[...], c_ref[...])
    own_ref[...] = own
    for k in range(n):
        out_ref[k] = own


def outer_body(_, hidden_ref, grad_ref, out_ref):
    blocks, rows, n = out_ref.shape
    share = lax.dot_general(
        grad_ref[...], hidden_ref[...], (((0,), (0,)), ((), ())), preferred_element_type=f32
    )
    out_ref[...] = (0.5 * share).astype(bf16).reshape(blocks, rows, n)


def own_rows_body(tp_ref, p0, p1, p2, p3, u_ref, c_ref, own_ref):
    rows = c_ref.shape[0]
    d_normed = p0[...].astype(f32)
    for p in (p1, p2, p3):
        d_normed = d_normed + p[...].astype(f32)
    u = u_ref[pl.ds(pl.multiple_of(tp_ref[0] * rows, rows), rows), :]
    own_ref[...] = gradient_of(d_normed, u, c_ref[...])


def place_rows_body(tp_ref, q0, q1, q2, q3, other_ref, out_ref):
    rows = q0.shape[0]
    x, core = tp_ref[0] // 2, lax.rem(tp_ref[0], 2)
    for j, q in enumerate((q0, q1, q2, q3)):
        at = lax.rem(x + j, 4) * 2
        out_ref[pl.ds(pl.multiple_of((at + core) * rows, rows), rows), :] = q[...]
        out_ref[pl.ds(pl.multiple_of((at + 1 - core) * rows, rows), rows), :] = other_ref[j]


SMEM = pl.BlockSpec(memory_space=pltpu.SMEM)
VMEM = pl.BlockSpec(memory_space=pltpu.VMEM)


def kernel(body, outs, flops, scalars, *arrays, scratch=(), near=()):
    arrays = [
        pltpu.with_memory_space_constraint(a, pltpu.MemorySpace.VMEM) if i in near else a
        for i, a in enumerate(arrays)
    ]
    return pl.pallas_call(
        body,
        in_specs=[SMEM] + [VMEM] * len(arrays),
        out_specs=tuple(VMEM for _ in outs),
        out_shape=tuple(jax.ShapeDtypeStruct(*o) for o in outs),
        scratch_shapes=scratch,
        cost_estimate=pl.CostEstimate(
            flops=flops, bytes_accessed=6 << 20, transcendentals=0
        ),
    )(scalars, *arrays)


def own_rows(partial):
    pieces = partial.reshape(lax.axis_size("tp"), -1, partial.shape[1])
    return lax.all_to_all(pieces, "tp", 0, 0, tiled=True)


def swap_cores(value):
    return lax.ppermute(value, "tp", [(i, i ^ 1) for i in range(lax.axis_size("tp"))])


def take_x(value, step):
    n = lax.axis_size("tp")
    return lax.ppermute(value, "tp", [((i + 2 * step) % n, i) for i in range(n)])


def own_rows_by_permutes(mine, other, x):
    other = swap_cores(other)
    chip = (mine.astype(f32) + other.astype(f32)).astype(bf16)

    def block(j):
        return lax.dynamic_index_in_dim(chip, (x + j) % 4, axis=0, keepdims=False)

    pieces = [block(0)]
    for j in (2, 1, 3):
        pieces.append(take_x(block(j), -j))
    return pieces


def all_rows(value, tps):
    quarters = [value]
    for j in (1, 2, 3):
        quarters.append(take_x(value, j))
    stacked = jnp.stack(quarters)
    other = swap_cores(stacked)
    out = ((8 * value.shape[0], value.shape[1]), bf16)
    (whole,) = kernel(place_rows_body, (out,), 1 << 20, tps, *quarters, other, near=range(5))
    return whole


def step(
    tokens,
    mid_tokens,
    out_grad,
    gate_first,
    up_first,
    down_first,
    gate_second,
    up_second,
    down_second,
):
    tp = lax.axis_index("tp")
    tps = tp.astype(jnp.int32).reshape(1)
    zs = jnp.stack([lax.axis_index("fs_0"), tp % 2]).astype(jnp.int32)
    n, width = gate_first.shape[1], tokens.shape[1]
    like_u = (tokens.shape, bf16)

    flops = 2 * tokens.shape[0] * width * n

    def packed(gate, up, down):
        out = ((lax.axis_size("fs_1"), gate.shape[0], 3 * n), bf16)
        return kernel(pack_body, (out,), 1 << 20, tps, gate, up, down.T)[0]

    def parts(whole):
        left = whole[:, :LEFT]
        return left, whole[:, LEFT:]

    y2 = along_y(packed(gate_second, up_second, down_second))
    y1 = packed(gate_first, up_first, down_first)
    y1 = along_y(after(y1, y2))
    a2, b2 = parts(y2)
    a1, b1 = parts(y1)
    a2 = along_z(a2, 1)
    b2 = along_z(b2, -1)
    a1 = along_z(a1, 1)
    b1 = along_z(b1, -1)

    sums, scale = kernel(
        near_body,
        (((tokens.shape[0], 3 * n), f32), ((tokens.shape[0], 128), f32)),
        2 * flops,
        zs,
        mid_tokens,
        out_grad,
        *a2[:3],
        *b2[:3],
    )
    (partial,) = kernel(
        block_body, (like_u,), 3 * flops, zs, mid_tokens, out_grad, sums, scale, *a2, *b2
    )
    pieces = own_rows(partial)
    rows, like_rows = pieces.shape[1], (pieces.shape[1:], bf16)
    u_rows = lax.dynamic_slice_in_dim(mid_tokens, tp * rows, rows, axis=0)
    c_rows = lax.dynamic_slice_in_dim(out_grad, tp * rows, rows, axis=0)
    mid_rows, spread = kernel(
        spread_rows_body,
        (like_rows, (pieces.shape, bf16)),
        1 << 24,
        tps,
        pieces,
        u_rows,
        c_rows,
        near=(0,),
    )
    mid_grad = lax.all_to_all(spread, "tp", 0, 0, tiled=True).reshape(mid_tokens.shape)

    sums_1, scale_1 = kernel(
        near_forward_body,
        (((tokens.shape[0], 2 * n), f32), ((tokens.shape[0], 128), f32)),
        flops,
        zs,
        tokens,
        *a1[:3],
        *b1[:3],
    )
    both, hidden = kernel(
        forward_body,
        (((tokens.shape[0], 2 * n), f32), ((tokens.shape[0], n), bf16)),
        flops,
        zs,
        tokens,
        sums_1,
        scale_1,
        a1[3],
        b1[3],
        near=(3, 4),
    )
    blocks = lax.axis_size(FS_REP)
    out = ((blocks, width // blocks, n), bf16)
    (share,) = kernel(outer_body, (out,), flops, tps, hidden, mid_grad, near=(1,))
    share = lax.all_to_all(share, FS_REP, 0, 0, tiled=True)
    share = share.astype(f32).sum(axis=0)
    twin = take_from(share, "rep", 1)
    norms = from_everyone(jnp.sum(share * share, axis=0), FS_REP)
    norms = norms.sum(axis=0)
    first = lax.axis_index("rep") == 0
    share = jnp.where(first, jnp.stack([share, twin]), jnp.stack([twin, share]))

    half = ((4, rows, width), bf16)
    mine, other = kernel(
        backward_body,
        (half, half),
        3 * flops,
        zs,
        mid_grad,
        both,
        *a1,
        *b1,
        scratch=[pltpu.VMEM(tokens.shape, bf16)],
    )
    pieces = own_rows_by_permutes(mine, other, tp // 2)
    (in_rows,) = kernel(
        own_rows_body, (like_rows,), 1 << 24, tps, *pieces, tokens, mid_rows, near=range(4)
    )
    input_grad = all_rows(in_rows, tps)
    return (input_grad, share.reshape(-1, n).T, norms)


def solution(mesh):
    torus = Mesh(
        mesh.devices.reshape(mesh.shape["rep"], 4, 8, mesh.shape["tp"]),
        ("rep", "fs_0", "fs_1", "tp"),
    )
    placed = (
        P(REP_FS, None),
        P(REP_FS, None),
        P(REP_FS, None),
        P(FS, "tp"),
        P(FS, "tp"),
        P("tp", FS),
        P(FS, "tp"),
        P(FS, "tp"),
        P("tp", FS),
    )
    return jax.shard_map(
        step,
        mesh=torus,
        in_specs=placed,
        out_specs=(P(REP_FS, None), P("tp", FS), P("tp")),
        check_vma=False,
    )
```

```python
import jax
import jax.numpy as jnp
from jax import lax
from jax.experimental import pallas as pl
from jax.experimental.pallas import tpu as pltpu
from jax.sharding import Mesh
from jax.sharding import PartitionSpec as P


FS = ("fs_0", "fs_1")
Z = ("rep", "fs_0")
REP_FS = ("rep", "fs_0", "fs_1")
FS_REP = ("fs_0", "fs_1", "rep")
f32 = jnp.float32
bf16 = jnp.bfloat16

eps = 1e-06
LEFT = 640
PIECES = (0, 1, 3, 2)
NEAR_2 = 2
ROWS_ROWS = (((1,), (1,)), ((), ()))


def take_from(value, axis, step):
    n = lax.axis_size(axis)
    return lax.ppermute(value, axis, [((i + step) % n, i) for i in range(n)])


def from_everyone(value, axis):
    n = lax.axis_size(axis)
    return lax.all_to_all(
        jnp.broadcast_to(value[None], (n, *value.shape)), axis, 0, 0, tiled=True
    )


def along_y(copies):
    whole = lax.all_to_all(copies, "fs_1", 0, 0, tiled=True)
    return whole.reshape(-1, copies.shape[2])


def along_z(value, forward):
    next_ = take_from(value, Z, 1)
    last = take_from(value, Z, -1)
    far = take_from(next_ if forward > 0 else last, Z, forward)
    return (value, next_, last, far)


def after(value, *others):
    return lax.optimization_barrier((value, *others))[0]


def span_of(z, m, width):
    quarter = width // 4
    return pl.ds(pl.multiple_of(lax.rem(z + m, 4) * quarter, quarter), quarter)


def pack_body(_, gate_ref, up_ref, down_ref, out_ref):
    n = gate_ref.shape[1]
    for k in range(out_ref.shape[0]):
        for j, ref in enumerate((gate_ref, up_ref, down_ref)):
            out_ref[k, :, j * n : (j + 1) * n] = ref[...]


def scale_of(u_ref):
    field = u_ref[...].astype(f32)
    return lax.rsqrt(jnp.mean(field * field, axis=1, keepdims=True) + eps)


def gate_up_of(z, u_ref, scale, places, left, right, n):
    width = u_ref.shape[1]
    a = b = None
    for m, wl, wr in zip(places, left, right):
        normed_b = (u_ref[:, span_of(z, m, width)].astype(f32) * scale).astype(bf16)
        part_a = jnp.dot(normed_b, wl[...], preferred_element_type=f32)
        part_b = jnp.dot(normed_b, wr[:, : 2 * n - LEFT], preferred_element_type=f32)
        a = part_a if a is None else a + part_a
        b = part_b if b is None else b + part_b
    return a, b


def back_of(z, c_ref, places, right, n):
    width = c_ref.shape[1]
    total = None
    for m, wr in zip(places, right):
        part = jnp.dot(
            c_ref[:, span_of(z, m, width)], wr[:, 2 * n - LEFT :], preferred_element_type=f32
        )
        total = part if total is None else total + part
    return total


def partial_of(z, back, gate, upper, left, right, out_ref):
    width, n = out_ref.shape[1], gate.shape[1]
    back = 0.5 * back
    logistic = jax.nn.sigmoid(gate)
    d_gate = (back * upper * logistic * (1.0 + gate * (1.0 - logistic))).astype(bf16)
    d_up = (back * (gate * logistic)).astype(bf16)
    d_left = jnp.concatenate([d_gate, d_up[:, : LEFT - n]], axis=1)
    d_right = d_up[:, LEFT - n :]
    for m, wl, wr in zip(PIECES, left, right):
        part = lax.dot_general(d_left, wl[...], ROWS_ROWS, preferred_element_type=f32)
        part = part + lax.dot_general(
            d_right, wr[:, : 2 * n - LEFT], ROWS_ROWS, preferred_element_type=f32
        )
        out_ref[:, span_of(z, m, width)] = part.astype(bf16)


def near_body(z_ref, u_ref, c_ref, *refs):
    *weight, sums_ref, scale_ref = refs
    k = len(weight) // 2
    z, left, right = z_ref[0], weight[:k], weight[k:]
    n = sums_ref.shape[1] // 3
    scale = scale_of(u_ref)
    a, b = gate_up_of(z, u_ref, scale, PIECES[:k], left, right, n)
    sums_ref[:, :LEFT] = a
    sums_ref[:, LEFT : 2 * n] = b
    sums_ref[:, 2 * n :] = back_of(z, c_ref, PIECES[:k], right, n)
    scale_ref[...] = jnp.broadcast_to(scale, scale_ref.shape)


def block_body(z_ref, u_ref, c_ref, sums_ref, scale_ref, *refs):
    *weight, out_ref = refs
    z, left, right = z_ref[0], weight[:4], weight[4:]
    n = sums_ref.shape[1] // 3
    k = NEAR_2
    a, b = gate_up_of(z, u_ref, scale_ref[:, :1], PIECES[k:], left[k:], right[k:], n)
    a, b = a + sums_ref[:, :LEFT], b + sums_ref[:, LEFT : 2 * n]
    back = back_of(z, c_ref, PIECES[k:], right[k:], n) + sums_ref[:, 2 * n :]
    upper = jnp.concatenate([a[:, n:], b], axis=1)
    partial_of(z, back, a[:, :n], upper, left, right, out_ref)


def near_forward_body(z_ref, u_ref, *refs):
    *weight, sums_ref, scale_ref = refs
    scale = scale_of(u_ref)
    n = sums_ref.shape[1] // 2
    a, b = gate_up_of(z_ref[0], u_ref, scale, PIECES[:3], weight[:3], weight[3:], n)
    sums_ref[:, :LEFT] = a
    sums_ref[:, LEFT:] = b
    scale_ref[...] = jnp.broadcast_to(scale, scale_ref.shape)


def forward_body(z_ref, u_ref, sums_ref, scale_ref, left_ref, right_ref, both_ref, hidden_ref):
    n = hidden_ref.shape[1]
    scale = scale_ref[:, :1]
    a, b = gate_up_of(z_ref[0], u_ref, scale, PIECES[3:], [left_ref], [right_ref], n)
    total = jnp.concatenate([a, b], axis=1) + sums_ref[...]
    gate, upper = total[:, :n], total[:, n:]
    both_ref[...] = total
    hidden_ref[...] = (gate * jax.nn.sigmoid(gate) * upper).astype(bf16)


def backward_body(z_ref, c_ref, both_ref, *refs):
    *weight, mine_ref, other_ref, out_ref = refs
    n = both_ref.shape[1] // 2
    gate, upper = both_ref[:, :n], both_ref[:, n:]
    back = back_of(z_ref[0], c_ref, PIECES, weight[4:], n)
    partial_of(z_ref[0], back, gate, upper, weight[:4], weight[4:], out_ref)
    core, (blocks, rows, _) = z_ref[1], mine_ref.shape
    for k in range(blocks):
        mine_ref[k] = out_ref[pl.ds(pl.multiple_of((2 * k + core) * rows, rows), rows), :]
        other_ref[k] = out_ref[pl.ds(pl.multiple_of((2 * k + 1 - core) * rows, rows), rows), :]


def gradient_of(d_normed, u, c):
    field = u.astype(f32)
    scale = lax.rsqrt(jnp.mean(field * field, axis=1, keepdims=True) + eps)
    normed = field * scale
    d_field = c.astype(f32) + scale * (
        d_normed - normed * jnp.mean(d_normed * normed, axis=1, keepdims=True)
    )
    return d_field.astype(bf16)


def spread_rows_body(tp_ref, p_ref, u_ref, c_ref, own_ref, out_ref):
    n, _, _ = p_ref.shape
    d_normed = p_ref[0].astype(f32)
    for k in range(1, n):
        d_normed = d_normed + p_ref[k].astype(f32)
    own = gradient_of(d_normed, u_ref[...], c_ref[...])
    own_ref[...] = own
    for k in range(n):
        out_ref[k] = own


def outer_body(_, hidden_ref, grad_ref, out_ref):
    blocks, rows, n = out_ref.shape
    share = lax.dot_general(
        grad_ref[...], hidden_ref[...], (((0,), (0,)), ((), ())), preferred_element_type=f32
    )
    out_ref[...] = (0.5 * share).astype(bf16).reshape(blocks, rows, n)


def own_rows_body(_, p0, p1, p2, p3, u_ref, c_ref, own_ref):
    d_normed = p0[...].astype(f32)
    for p in (p1, p2, p3):
        d_normed = d_normed + p[...].astype(f32)
    own_ref[...] = gradient_of(d_normed, u_ref[...], c_ref[...])


def place_rows_body(tp_ref, q0, q1, q2, q3, other_ref, out_ref):
    rows = q0.shape[0]
    x, core = tp_ref[0] // 2, lax.rem(tp_ref[0], 2)
    for j, q in enumerate((q0, q1, q2, q3)):
        at = lax.rem(x + j, 4) * 2
        out_ref[pl.ds(pl.multiple_of((at + core) * rows, rows), rows), :] = q[...]
        out_ref[pl.ds(pl.multiple_of((at + 1 - core) * rows, rows), rows), :] = other_ref[j]


SMEM = pl.BlockSpec(memory_space=pltpu.SMEM)
VMEM = pl.BlockSpec(memory_space=pltpu.VMEM)


def kernel(body, outs, flops, scalars, *arrays, scratch=(), near=()):
    arrays = [
        pltpu.with_memory_space_constraint(a, pltpu.MemorySpace.VMEM) if i in near else a
        for i, a in enumerate(arrays)
    ]
    return pl.pallas_call(
        body,
        in_specs=[SMEM] + [VMEM] * len(arrays),
        out_specs=tuple(VMEM for _ in outs),
        out_shape=tuple(jax.ShapeDtypeStruct(*o) for o in outs),
        scratch_shapes=scratch,
        cost_estimate=pl.CostEstimate(
            flops=flops, bytes_accessed=6 << 20, transcendentals=0
        ),
    )(scalars, *arrays)


def own_rows(partial):
    pieces = partial.reshape(lax.axis_size("tp"), -1, partial.shape[1])
    return lax.all_to_all(pieces, "tp", 0, 0, tiled=True)


def swap_cores(value):
    return lax.ppermute(value, "tp", [(i, i ^ 1) for i in range(lax.axis_size("tp"))])


def take_x(value, step):
    n = lax.axis_size("tp")
    return lax.ppermute(value, "tp", [((i + 2 * step) % n, i) for i in range(n)])


def own_rows_by_permutes(mine, other, x):
    other = swap_cores(other)
    chip = (mine.astype(f32) + other.astype(f32)).astype(bf16)

    def block(j):
        return lax.dynamic_index_in_dim(chip, (x + j) % 4, axis=0, keepdims=False)

    pieces = [block(0)]
    for j in (2, 1, 3):
        pieces.append(take_x(block(j), -j))
    return pieces


def all_rows(value, tps):
    quarters = [value]
    for j in (1, 2, 3):
        quarters.append(take_x(value, j))
    stacked = jnp.stack(quarters)
    other = swap_cores(stacked)
    out = ((8 * value.shape[0], value.shape[1]), bf16)
    (whole,) = kernel(place_rows_body, (out,), 1 << 20, tps, *quarters, other, near=range(5))
    return whole


def step(
    tokens,
    mid_tokens,
    out_grad,
    gate_first,
    up_first,
    down_first,
    gate_second,
    up_second,
    down_second,
):
    tp = lax.axis_index("tp")
    tps = tp.astype(jnp.int32).reshape(1)
    zs = jnp.stack([lax.axis_index("fs_0"), tp % 2]).astype(jnp.int32)
    n, width = gate_first.shape[1], tokens.shape[1]
    like_u = (tokens.shape, bf16)

    flops = 2 * tokens.shape[0] * width * n

    def packed(gate, up, down):
        out = ((lax.axis_size("fs_1"), gate.shape[0], 3 * n), bf16)
        return kernel(pack_body, (out,), 1 << 20, tps, gate, up, down.T)[0]

    def parts(whole):
        left = whole[:, :LEFT]
        return left, whole[:, LEFT:]

    y2 = along_y(packed(gate_second, up_second, down_second))
    y1 = packed(gate_first, up_first, down_first)
    y1 = along_y(after(y1, y2))
    a2, b2 = parts(y2)
    a1, b1 = parts(y1)
    a2 = along_z(a2, 1)
    b2 = along_z(b2, -1)
    a1 = along_z(a1, 1)
    b1 = along_z(b1, -1)

    sums, scale = kernel(
        near_body,
        (((tokens.shape[0], 3 * n), f32), ((tokens.shape[0], 128), f32)),
        2 * flops,
        zs,
        mid_tokens,
        out_grad,
        *a2[:NEAR_2],
        *b2[:NEAR_2],
    )
    (partial,) = kernel(
        block_body, (like_u,), 3 * flops, zs, mid_tokens, out_grad, sums, scale, *a2, *b2
    )
    pieces = own_rows(partial)
    rows, like_rows = pieces.shape[1], (pieces.shape[1:], bf16)
    u_rows = lax.dynamic_slice_in_dim(mid_tokens, tp * rows, rows, axis=0)
    c_rows = lax.dynamic_slice_in_dim(out_grad, tp * rows, rows, axis=0)
    own_tokens = lax.dynamic_slice_in_dim(tokens, tp * rows, rows, axis=0)
    mid_rows, spread = kernel(
        spread_rows_body,
        (like_rows, (pieces.shape, bf16)),
        1 << 24,
        tps,
        pieces,
        u_rows,
        c_rows,
        near=(0,),
    )
    mid_grad = lax.all_to_all(spread, "tp", 0, 0, tiled=True).reshape(mid_tokens.shape)

    sums_1, scale_1 = kernel(
        near_forward_body,
        (((tokens.shape[0], 2 * n), f32), ((tokens.shape[0], 128), f32)),
        flops,
        zs,
        tokens,
        *a1[:3],
        *b1[:3],
    )
    both, hidden = kernel(
        forward_body,
        (((tokens.shape[0], 2 * n), f32), ((tokens.shape[0], n), bf16)),
        flops,
        zs,
        tokens,
        sums_1,
        scale_1,
        a1[3],
        b1[3],
        near=(3, 4),
    )
    blocks = lax.axis_size(FS_REP)
    out = ((blocks, width // blocks, n), bf16)
    (share,) = kernel(outer_body, (out,), flops, tps, hidden, mid_grad, near=(0, 1))
    share = lax.all_to_all(share, FS_REP, 0, 0, tiled=True)
    share = share.astype(f32).sum(axis=0)
    twin = take_from(share, "rep", 1)
    norms = from_everyone(jnp.sum(share * share, axis=0), FS_REP)
    norms = norms.sum(axis=0)
    first = lax.axis_index("rep") == 0
    share = jnp.where(first, jnp.stack([share, twin]), jnp.stack([twin, share]))

    half = ((4, rows, width), bf16)
    mine, other = kernel(
        backward_body,
        (half, half),
        3 * flops,
        zs,
        mid_grad,
        both,
        *a1,
        *b1,
        scratch=[pltpu.VMEM(tokens.shape, bf16)],
    )
    pieces = own_rows_by_permutes(mine, other, tp // 2)
    (in_rows,) = kernel(
        own_rows_body, (like_rows,), 1 << 24, tps, *pieces, own_tokens, mid_rows, near=range(4)
    )
    input_grad = all_rows(in_rows, tps)
    return (input_grad, share.reshape(-1, n).T, norms)


def solution(mesh):
    torus = Mesh(
        mesh.devices.reshape(mesh.shape["rep"], 4, 8, mesh.shape["tp"]),
        ("rep", "fs_0", "fs_1", "tp"),
    )
    placed = (
        P(REP_FS, None),
        P(REP_FS, None),
        P(REP_FS, None),
        P(FS, "tp"),
        P(FS, "tp"),
        P("tp", FS),
        P(FS, "tp"),
        P(FS, "tp"),
        P("tp", FS),
    )
    return jax.shard_map(
        step,
        mesh=torus,
        in_specs=placed,
        out_specs=(P(REP_FS, None), P("tp", FS), P("tp")),
        check_vma=False,
    )
```
